32 devices in a mesh: fs: 8 (over z, y), tp: 4 (over x, core).
Axes of the slice: x: 2, y: 2, z: 4, core: 2. Of those that a mesh axis runs over, the one named last changes fastest.
Arguments:
- prompt_tokens: bfloat16 [4, 128, 4096], P('tp'), may hold values from -6 to 6
- trained_up: float32 [4096, 16384], P('fs', 'tp'), may hold values from -0.09375 to 0.09375
- trained_down: float32 [16384, 4096], P('fs', 'tp'), may hold values from -0.046875 to 0.046875
- pre_gain: float32 [4096], P('fs'), may hold values from 0.1 to 1.9
- post_gain: float32 [4096], replicated, may hold values from 0.1 to 1.9
Outputs:
- layer_out: bfloat16 [4, 128, 4096], P('tp', 'fs')
- sampler_up: bfloat16 [4096, 16384], P(None, 'fs')
- sampler_down: bfloat16 [16384, 4096], P('fs')
The draws below stay inside these ranges and needn't reach their ends.
All inputs are finite; a program needn't handle non-finite values.
Results may differ from the reference program's by a relative error of at most 0.0081.
Values may be sent and summed in bfloat16 or wider, within the bound.
A program may use at most 128 MiB of HBM per device.

```python
import jax
import jax.numpy as jnp
from jax import lax

D = 4096
FF = 16384
TOK_G = 128
N_TP = 4


def steps_of(rng, dims, pieces, least, top_value):
    factor_of = 1.0
    for position, shards_of in pieces:
        heights = jax.random.uniform(jax.random.fold_in(jax.random.fold_in(rng, 6), position), (shards_of,), jnp.float32, least / len(pieces), top_value / len(pieces))
        factor_of = factor_of * jnp.repeat(jnp.exp(heights), dims[position] // shards_of).reshape((-1,) + (1,) * (len(dims) - 1 - position))
    return factor_of


def gaussian(own_key, shape, scale, reach, cuts=(), held_as=jnp.bfloat16):
    values = jax.random.normal(own_key, shape, jnp.float32) * scale
    if len(cuts) > 0:
        values = steps_of(own_key, shape, cuts, -0.22, 0.18) * values
    return jnp.clip(values, min=-reach, max=reach).astype(held_as)


def setup_inputs(seed: int = 0) -> dict:
    keys = jax.random.split(jax.random.key(seed), 6)
    return {
        "prompt_tokens": gaussian(keys[0], (N_TP, TOK_G, D), 1.0, 6.0, ((0, 4),)),
        "trained_up": gaussian(keys[1], (D, FF), D ** -0.5, 0.09375, ((0, 8), (1, 4)), jnp.float32),
        "trained_down": gaussian(keys[2], (FF, D), FF ** -0.5, 0.046875, ((0, 8), (1, 4)), jnp.float32),
        "pre_gain": jnp.clip(1.0 + 0.18 * jax.random.normal(keys[3], (D,), jnp.float32), 0.1, 1.9),
        "post_gain": jnp.clip(1.0 + 0.18 * jax.random.normal(keys[4], (D,), jnp.float32), 0.1, 1.9),
    }


def row_norm(values):
    return values * lax.rsqrt(lax.optimization_barrier(jnp.mean(values * values, axis=-1, keepdims=True)) + 1e-06)

def reference(prompt_tokens, trained_up, trained_down, pre_gain, post_gain):
    sampler_up = (pre_gain[:, None] * trained_up).astype(jnp.bfloat16)
    sampler_down = trained_down.astype(jnp.bfloat16)
    flat = prompt_tokens.reshape(-1, prompt_tokens.shape[-1]).astype(jnp.float32)
    normed = row_norm(flat).astype(jnp.bfloat16)
    upward = jnp.dot(normed, sampler_up, preferred_element_type=jnp.float32)
    hidden = jnp.square(jax.nn.relu(upward)).astype(jnp.bfloat16)
    summed = jnp.dot(hidden, sampler_down, preferred_element_type=jnp.float32)
    layer_out = (row_norm(summed) * post_gain).astype(jnp.bfloat16)
    return (layer_out.reshape(prompt_tokens.shape), sampler_up, sampler_down)
```

```python
import functools

import jax
import jax.numpy as jnp
from jax import lax
from jax.experimental import pallas as pl
from jax.experimental.pallas import tpu as pltpu
from jax.sharding import PartitionSpec as P

MESH = pl.DeviceIdType.MESH
EPS = 1e-06


def remote(src, dst, send_sem, recv_sem, device):
    return pltpu.make_async_remote_copy(
        src_ref=src, dst_ref=dst, send_sem=send_sem, recv_sem=recv_sem, device_id=device, device_id_type=MESH
    )


def greet(device):
    pl.semaphore_signal(pltpu.get_barrier_semaphore(), inc=1, device_id=device, device_id_type=MESH)


def loop(count, body):
    lax.fori_loop(0, count, lambda i, c: (body(i), c)[1], 0)


def spread_kernel(
    n_fs, n_tp, n_r,
    up, down, gup, gdown, xup,
    xs, xr, ps, pr, ws, wr, ns, nr, ls, ds, dr, vs, vr,
):
    f, t = lax.axis_index("fs"), lax.axis_index("tp")
    far = lax.rem(t + n_tp // 2, n_tp)
    near = t + 1 - 2 * lax.rem(t, 2)
    near_far = lax.rem(near + n_tp // 2, n_tp)
    m = n_fs // n_tp
    rows, width = up.shape[0], up.shape[1] // m
    part = rows // n_r
    d_rows, d_width = down.shape
    d_part = d_rows // n_r
    pieces = m * n_r
    active = lax.rem(lax.rem(f // m, 2) + lax.rem(t, 2), 2) == 0

    def piece(ref, k):
        r, j = k // m, lax.rem(k, m)
        return ref.at[pl.ds(pl.multiple_of(r * part, part), part), pl.ds(pl.multiple_of(j * width, width), width)]

    def landed(source, r):
        return gup.at[pl.ds(pl.multiple_of(source * rows + r * part, part), part), :]

    def x_copy(k):
        return remote(piece(up, k), piece(xup, k), xs.at[k], xr.at[k], {"tp": far})

    def owner(phase, k):
        return (t if phase == 0 else far) * m + lax.rem(k, m)

    def peer_copy(phase, k):
        held = up if phase == 0 else xup
        return remote(piece(held, k), landed(f, k // m), ps.at[phase, k], pr.at[f, k // m], {"fs": owner(phase, k)})

    def start_peer(phase, k):
        mine = owner(phase, k) == f

        @pl.when(mine)
        def _():
            held = up if phase == 0 else xup
            pltpu.make_async_copy(piece(held, k), landed(f, k // m), pr.at[f, k // m]).start()

        @pl.when(jnp.logical_not(mine))
        def _():
            peer_copy(phase, k).start()

    def end_peer(phase, k):
        @pl.when(owner(phase, k) != f)
        def _():
            peer_copy(phase, k).wait_send()

    def block(q, which):
        return gdown.at[
            pl.ds(pl.multiple_of(q * d_part, d_part), d_part), pl.ds(pl.multiple_of(which * d_width, d_width), d_width)
        ]

    def columns(which):
        return gdown.at[:, pl.ds(pl.multiple_of(which * d_width, d_width), d_width)]

    def d_copy(q):
        return remote(
            down.at[pl.ds(pl.multiple_of(q * d_part, d_part), d_part), :], block(q, t), ds.at[q], dr.at[q], {"tp": far}
        )

    def d_pass(q, which):
        return remote(block(q, which), block(q, which), vs.at[q], vr.at[q], {"tp": near})

    def share(source, r):
        return remote(landed(source, r), landed(source, r), ws.at[source, r], wr.at[source, r], {"tp": near})

    loop(n_fs - 1, lambda i: greet({"fs": lax.rem(f + 1 + i, n_fs)}))
    greet({"tp": far})
    greet({"tp": near})
    pl.semaphore_wait(pltpu.get_barrier_semaphore(), n_fs + 1)

    loop(pieces, lambda k: x_copy(k).start())
    loop(pieces, lambda k: start_peer(0, k))
    to_near = remote(down, columns(t), ns, nr, {"tp": near})
    to_near.start()
    own = pltpu.make_async_copy(down, columns(t), ls)
    own.start()

    def pass_on(k):
        @pl.when(k == pieces - 1)
        def _():
            loop(n_r, lambda q: d_copy(q).start())

        x_copy(k).wait_recv()
        start_peer(1, k)

    loop(pieces, pass_on)

    def gather(r):
        @pl.when(active)
        def _():
            def one(source):
                @pl.when(source == f)
                def _():
                    pltpu.make_async_copy(landed(f, r), landed(f, r), pr.at[f, r]).wait()

                @pl.when(source != f)
                def _():
                    remote(landed(source, r), landed(source, r), ws.at[source, r], pr.at[source, r], {"tp": near}).wait_recv()

                share(source, r).start()

            loop(n_fs, one)

        remote(block(r, far), block(r, far), ds.at[r], dr.at[r], {"tp": far}).wait_recv()
        d_pass(r, far).start()

    loop(n_r, gather)

    def ended(i):
        source, r = i // n_r, lax.rem(i, n_r)

        @pl.when(active)
        def _():
            share(source, r).wait_send()

        @pl.when(jnp.logical_not(active))
        def _():
            share(source, r).wait_recv()

    loop(n_fs * n_r, ended)
    own.wait()
    to_near.wait_send()
    remote(columns(near), columns(near), ns, nr, {"tp": near}).wait_recv()

    def ended_down(q):
        d_copy(q).wait_send()
        d_pass(q, far).wait_send()
        d_pass(q, near_far).wait_recv()

    loop(n_r, ended_down)

    def ended_pieces(k):
        x_copy(k).wait_send()
        end_peer(0, k)
        end_peer(1, k)

    loop(pieces, ended_pieces)


def layer_kernel(tokens, up, down, part_out, up_out, down_out, normed, total):
    step = pl.program_id(0)

    @pl.when(step == 0)
    def _():
        flat = tokens[...].astype(jnp.float32)
        normed[...] = (flat * lax.rsqrt(jnp.mean(flat * flat, axis=-1, keepdims=True) + EPS)).astype(jnp.bfloat16)
        total[...] = jnp.zeros_like(total)

    up_out[...] = up[...]
    down_out[...] = down[...]
    upward = jnp.dot(normed[...], up[...], preferred_element_type=jnp.float32)
    hidden = jnp.square(jnp.maximum(upward, 0.0)).astype(jnp.bfloat16)
    total[...] += jnp.dot(hidden, down[...], preferred_element_type=jnp.float32)

    @pl.when(step == pl.num_programs(0) - 1)
    def _():
        part_out[...] = total[...].astype(part_out.dtype)


def sum_kernel(n_fs, parts, gain, out, land, ss, rs):
    f = lax.axis_index("fs")

    def peer_of(i):
        return lax.rem(f + 1 + i, n_fs)

    loop(n_fs - 1, lambda i: greet({"fs": peer_of(i)}))
    pl.semaphore_wait(pltpu.get_barrier_semaphore(), n_fs - 1)

    def send(i):
        return remote(parts.at[peer_of(i)], land.at[f], ss.at[i], rs.at[f], {"fs": peer_of(i)})

    loop(n_fs - 1, lambda i: send(i).start())

    def add(i, total):
        source = peer_of(i)
        remote(land.at[source], land.at[source], ss.at[i], rs.at[source], {"fs": source}).wait_recv()
        return total + land[source].astype(jnp.float32)

    summed = lax.fori_loop(0, n_fs - 1, add, parts[f].astype(jnp.float32))
    scale = lax.rsqrt(jnp.mean(summed * summed, axis=-1, keepdims=True) + EPS)
    out[...] = (summed * scale * gain[...]).astype(out.dtype)
    loop(n_fs - 1, lambda i: send(i).wait_send())


def on_device(n_fs, n_tp, prompt_tokens, trained_up, trained_down, pre_gain, post_gain):
    bf16 = jnp.bfloat16
    up = (pre_gain[:, None] * trained_up).astype(bf16)
    down = trained_down.astype(bf16)
    rows, cols = up.shape
    d_rows, d_cols = down.shape
    tokens, width = prompt_tokens.shape[1:]
    m = n_fs // n_tp
    owned = cols // m
    n_r = max(1, rows // 128)
    pieces = m * n_r
    anywhere = pl.BlockSpec(memory_space=pl.ANY)
    vmem = pl.BlockSpec(memory_space=pltpu.VMEM)
    dma = pltpu.SemaphoreType.DMA
    gup, gdown = pl.pallas_call(
        functools.partial(spread_kernel, n_fs, n_tp, n_r),
        out_shape=(
            jax.ShapeDtypeStruct((n_fs * rows, owned), bf16),
            jax.ShapeDtypeStruct((d_rows, n_tp * d_cols), bf16),
        ),
        in_specs=[vmem, vmem],
        out_specs=(anywhere, anywhere),
        scratch_shapes=[
            pltpu.VMEM(up.shape, bf16),
            dma((pieces,)), dma((pieces,)),
            dma((2, pieces)), dma((n_fs, n_r)),
            dma((n_fs, n_r)), dma((n_fs, n_r)),
            dma, dma, dma,
            dma((n_r,)), dma((n_r,)),
            dma((n_r,)), dma((n_r,)),
        ],
        compiler_params=pltpu.CompilerParams(collective_id=0, has_side_effects=True),
    )(up, down)

    tile = min(owned, 256)
    parts, sampler_up, sampler_down = pl.pallas_call(
        layer_kernel,
        grid=(owned // tile,),
        out_shape=(
            jax.ShapeDtypeStruct((tokens, width), bf16),
            jax.ShapeDtypeStruct(gup.shape, bf16),
            jax.ShapeDtypeStruct(gdown.shape, bf16),
        ),
        in_specs=[
            pl.BlockSpec((tokens, width), lambda i: (0, 0)),
            pl.BlockSpec((gup.shape[0], tile), lambda i: (0, i)),
            pl.BlockSpec((tile, gdown.shape[1]), lambda i: (i, 0)),
        ],
        out_specs=(
            pl.BlockSpec((tokens, width), lambda i: (0, 0)),
            pl.BlockSpec((gup.shape[0], tile), lambda i: (0, i)),
            pl.BlockSpec((tile, gdown.shape[1]), lambda i: (i, 0)),
        ),
        scratch_shapes=[pltpu.VMEM((tokens, width), bf16), pltpu.VMEM((tokens, width), jnp.float32)],
    )(prompt_tokens[0], gup, gdown)

    share = tokens // n_fs
    layer_out = pl.pallas_call(
        functools.partial(sum_kernel, n_fs),
        out_shape=jax.ShapeDtypeStruct((share, width), bf16),
        in_specs=[vmem, vmem],
        out_specs=vmem,
        scratch_shapes=[pltpu.VMEM((n_fs, share, width), bf16), dma((n_fs - 1,)), dma((n_fs,))],
        compiler_params=pltpu.CompilerParams(collective_id=1, has_side_effects=True),
    )(parts.reshape(n_fs, share, width), post_gain[None])
    return (layer_out[None], sampler_up, sampler_down)


def solution(mesh):
    placed = (P("tp", None, None), P("fs", "tp"), P("fs", "tp"), P("fs"), P())
    return jax.shard_map(
        functools.partial(on_device, mesh.shape["fs"], mesh.shape["tp"]),
        mesh=mesh,
        in_specs=placed,
        out_specs=(P("tp", "fs", None), P(None, "fs"), P("fs", None)),
        check_vma=False,
    )
```

```python
import functools

import jax
import jax.numpy as jnp
from jax import lax
from jax.experimental import pallas as pl
from jax.experimental.pallas import tpu as pltpu
from jax.sharding import PartitionSpec as P

MESH = pl.DeviceIdType.MESH
EPS = 1e-06


def remote(src, dst, send_sem, recv_sem, device):
    return pltpu.make_async_remote_copy(
        src_ref=src, dst_ref=dst, send_sem=send_sem, recv_sem=recv_sem, device_id=device, device_id_type=MESH
    )


def greet(device):
    pl.semaphore_signal(pltpu.get_barrier_semaphore(), inc=1, device_id=device, device_id_type=MESH)


def loop(count, body):
    lax.fori_loop(0, count, lambda i, c: (body(i), c)[1], 0)


def spread_kernel(
    n_fs, n_tp, n_r,
    up, down, tokens, gup, gdown, parts, held_up, held_down, xup, normed, upward, hidden,
    xs, xr, ps, pr, ws, wr, ns, nr, us, ls, ds, dr, vs, vr,
):
    f, t = lax.axis_index("fs"), lax.axis_index("tp")
    far = lax.rem(t + n_tp // 2, n_tp)
    near = t + 1 - 2 * lax.rem(t, 2)
    near_far = lax.rem(near + n_tp // 2, n_tp)
    m = n_fs // n_tp
    rows, width = up.shape[0], up.shape[1] // m
    part = rows // n_r
    d_rows, d_width = down.shape
    d_part = d_rows // n_r
    pieces = m * n_r
    block_of_f = f // m
    active = lax.rem(lax.rem(block_of_f, 2) + lax.rem(t, 2), 2) == 0

    def piece_at(r, j):
        return (
            pl.ds(pl.multiple_of(r * part, part), part),
            pl.ds(pl.multiple_of(j * width, width), width),
        )

    def piece(ref, k):
        return ref.at[piece_at(k // m, lax.rem(k, m))]

    def rows_of(source, r):
        return pl.ds(pl.multiple_of(source * rows + r * part, part), part)

    def landed(source, r):
        return held_up.at[rows_of(source, r)]

    def x_copy(k):
        return remote(piece(up, k), piece(xup, k), xs.at[k], xr.at[k], {"tp": far})

    def owner(phase, k):
        return (t if phase == 0 else far) * m + lax.rem(k, m)

    def peer_copy(phase, k):
        held = up if phase == 0 else xup
        return remote(piece(held, k), landed(f, k // m), ps.at[phase, k], pr.at[f, k // m], {"fs": owner(phase, k)})

    def start_peer(phase, k):
        @pl.when(owner(phase, k) != f)
        def _():
            peer_copy(phase, k).start()

    def end_peer(phase, k):
        @pl.when(owner(phase, k) != f)
        def _():
            peer_copy(phase, k).wait_send()

    def d_rows_of(q):
        return pl.ds(pl.multiple_of(q * d_part, d_part), d_part)

    def columns(which):
        return pl.ds(pl.multiple_of(which * d_width, d_width), d_width)

    def block(q, which):
        return held_down.at[which, d_rows_of(q)]

    def d_copy(q):
        return remote(down.at[d_rows_of(q)], block(q, t), ds.at[q], dr.at[q], {"tp": far})

    def d_pass(q, which):
        return remote(block(q, which), block(q, which), vs.at[q], vr.at[q], {"tp": near})

    def d_put(q, which):
        pltpu.make_async_copy(block(q, which), gdown.at[d_rows_of(q), columns(which)], ls).start()

    def share(src, source, r):
        return remote(src, landed(source, r), ws.at[source, r], wr.at[source, r], {"tp": near})

    def put(src, source, r):
        pltpu.make_async_copy(src, gup.at[rows_of(source, r)], us).start()

    loop(n_fs - 1, lambda i: greet({"fs": lax.rem(f + 1 + i, n_fs)}))
    greet({"tp": far})
    greet({"tp": near})
    pl.semaphore_wait(pltpu.get_barrier_semaphore(), n_fs + 1)

    loop(pieces, lambda k: x_copy(k).start())
    loop(pieces, lambda k: start_peer(0, k))
    to_near = remote(down, held_down.at[t], ns, nr, {"tp": near})
    to_near.start()
    pltpu.make_async_copy(down, gdown.at[:, columns(t)], ls).start()

    flat = tokens[...].astype(jnp.float32)
    scaled = (flat * lax.rsqrt(jnp.mean(flat * flat, axis=-1, keepdims=True) + EPS)).astype(jnp.bfloat16)
    for i in range(n_fs * n_r):
        normed[i] = scaled[:, i * part : (i + 1) * part]
    upward[...] = jnp.zeros_like(upward)

    def keep_down(q):
        held_down[t, d_rows_of(q)] = down[d_rows_of(q)]

    loop(n_r, keep_down)

    def pass_on(k):
        @pl.when(k == pieces - 1)
        def _():
            loop(n_r, lambda q: d_copy(q).start())

        x_copy(k).wait_recv()
        start_peer(1, k)

    loop(pieces, pass_on)

    def gather(r):
        def one(source):
            def keep_own(held):
                src = held.at[piece_at(r, lax.rem(f, m))]
                share(src, source, r).start()
                put(src, source, r)
                held_up[rows_of(source, r)] = held[piece_at(r, lax.rem(f, m))]

            @pl.when(jnp.logical_and(active, source == f))
            def _():
                @pl.when(block_of_f == t)
                def _():
                    keep_own(up)

                @pl.when(block_of_f != t)
                def _():
                    keep_own(xup)

            @pl.when(jnp.logical_and(active, source != f))
            def _():
                remote(landed(source, r), landed(source, r), ws.at[source, r], pr.at[source, r], {"tp": near}).wait_recv()
                share(landed(source, r), source, r).start()
                put(landed(source, r), source, r)

            @pl.when(jnp.logical_not(active))
            def _():
                share(landed(source, r), source, r).wait_recv()
                put(landed(source, r), source, r)

            upward[...] += jnp.dot(
                normed[source * n_r + r], held_up[rows_of(source, r)], preferred_element_type=jnp.float32
            )

        loop(n_fs, one)
        remote(block(r, far), block(r, far), ds.at[r], dr.at[r], {"tp": far}).wait_recv()
        d_pass(r, far).start()
        d_put(r, far)
        d_pass(r, near_far).wait_recv()
        d_put(r, near_far)

    loop(n_r, gather)
    remote(held_down.at[near], held_down.at[near], ns, nr, {"tp": near}).wait_recv()
    pltpu.make_async_copy(held_down.at[near], gdown.at[:, columns(near)], ls).start()

    hidden[...] = jnp.square(jnp.maximum(upward[...], 0.0)).astype(jnp.bfloat16)
    tile = min(d_width, 256)
    per_block = d_width // tile

    def finish(i):
        b, j = i // per_block, lax.rem(i, per_block)
        parts[:, pl.ds(pl.multiple_of(i * tile, tile), tile)] = jnp.dot(
            hidden[...],
            held_down[b, :, pl.ds(pl.multiple_of(j * tile, tile), tile)],
            preferred_element_type=jnp.float32,
        ).astype(parts.dtype)

    loop(n_tp * per_block, finish)

    def ended(i):
        @pl.when(active)
        def _():
            source, r = i // n_r, lax.rem(i, n_r)
            share(landed(source, r), source, r).wait_send()

    loop(n_fs * n_r, ended)
    to_near.wait_send()

    def ended_down(q):
        d_copy(q).wait_send()
        d_pass(q, far).wait_send()

    loop(n_r, ended_down)

    def ended_pieces(k):
        x_copy(k).wait_send()
        end_peer(0, k)
        end_peer(1, k)

    loop(pieces, ended_pieces)
    pltpu.make_async_copy(held_up, gup, us).wait()
    pltpu.make_async_copy(gdown, gdown, ls).wait()


def copy_kernel(up, down, up_out, down_out):
    up_out[...] = up[...]
    down_out[...] = down[...]


def sum_kernel(n_fs, parts, gain, out, land, ss, rs):
    f = lax.axis_index("fs")

    def peer_of(i):
        return lax.rem(f + 1 + i, n_fs)

    loop(n_fs - 1, lambda i: greet({"fs": peer_of(i)}))
    pl.semaphore_wait(pltpu.get_barrier_semaphore(), n_fs - 1)

    def send(i):
        return remote(parts.at[peer_of(i)], land.at[f], ss.at[i], rs.at[f], {"fs": peer_of(i)})

    loop(n_fs - 1, lambda i: send(i).start())

    def add(i, total):
        source = peer_of(i)
        remote(land.at[source], land.at[source], ss.at[i], rs.at[source], {"fs": source}).wait_recv()
        return total + land[source].astype(jnp.float32)

    summed = lax.fori_loop(0, n_fs - 1, add, parts[f].astype(jnp.float32))
    scale = lax.rsqrt(jnp.mean(summed * summed, axis=-1, keepdims=True) + EPS)
    out[...] = (summed * scale * gain[...]).astype(out.dtype)
    loop(n_fs - 1, lambda i: send(i).wait_send())


def on_device(n_fs, n_tp, prompt_tokens, trained_up, trained_down, pre_gain, post_gain):
    bf16 = jnp.bfloat16
    up = (pre_gain[:, None] * trained_up).astype(bf16)
    down = trained_down.astype(bf16)
    rows, cols = up.shape
    d_rows, d_cols = down.shape
    tokens, width = prompt_tokens.shape[1:]
    m = n_fs // n_tp
    owned = cols // m
    n_r = max(1, rows // 128)
    pieces = m * n_r
    anywhere = pl.BlockSpec(memory_space=pl.ANY)
    vmem = pl.BlockSpec(memory_space=pltpu.VMEM)
    dma = pltpu.SemaphoreType.DMA
    gup, gdown, parts = pl.pallas_call(
        functools.partial(spread_kernel, n_fs, n_tp, n_r),
        out_shape=(
            jax.ShapeDtypeStruct((n_fs * rows, owned), bf16),
            jax.ShapeDtypeStruct((d_rows, n_tp * d_cols), bf16),
            jax.ShapeDtypeStruct((tokens, width), bf16),
        ),
        in_specs=[vmem, vmem, vmem],
        out_specs=(anywhere, anywhere, vmem),
        scratch_shapes=[
            pltpu.VMEM((n_fs * rows, owned), bf16),
            pltpu.VMEM((n_tp, d_rows, d_cols), bf16),
            pltpu.VMEM(up.shape, bf16),
            pltpu.VMEM((n_fs * n_r, tokens, rows // n_r), bf16),
            pltpu.VMEM((tokens, owned), jnp.float32),
            pltpu.VMEM((tokens, owned), bf16),
            dma((pieces,)), dma((pieces,)),
            dma((2, pieces)), dma((n_fs, n_r)),
            dma((n_fs, n_r)), dma((n_fs, n_r)),
            dma, dma, dma, dma,
            dma((n_r,)), dma((n_r,)),
            dma((n_r,)), dma((n_r,)),
        ],
        compiler_params=pltpu.CompilerParams(collective_id=0, has_side_effects=True, vmem_limit_bytes=64000000),
    )(up, down, prompt_tokens[0])

    steps = 8
    blocks = [
        pl.BlockSpec((gup.shape[0] // steps, owned), lambda i: (i, 0)),
        pl.BlockSpec((d_rows // steps, gdown.shape[1]), lambda i: (i, 0)),
    ]
    sampler_up, sampler_down = pl.pallas_call(
        copy_kernel,
        grid=(steps,),
        out_shape=(jax.ShapeDtypeStruct(gup.shape, bf16), jax.ShapeDtypeStruct(gdown.shape, bf16)),
        in_specs=blocks,
        out_specs=tuple(blocks),
    )(gup, gdown)

    share = tokens // n_fs
    layer_out = pl.pallas_call(
        functools.partial(sum_kernel, n_fs),
        out_shape=jax.ShapeDtypeStruct((share, width), bf16),
        in_specs=[vmem, vmem],
        out_specs=vmem,
        scratch_shapes=[pltpu.VMEM((n_fs, share, width), bf16), dma((n_fs - 1,)), dma((n_fs,))],
        compiler_params=pltpu.CompilerParams(collective_id=1, has_side_effects=True),
    )(parts.reshape(n_fs, share, width), post_gain[None])
    return (layer_out[None], sampler_up, sampler_down)


def solution(mesh):
    placed = (P("tp", None, None), P("fs", "tp"), P("fs", "tp"), P("fs"), P())
    return jax.shard_map(
        functools.partial(on_device, mesh.shape["fs"], mesh.shape["tp"]),
        mesh=mesh,
        in_specs=placed,
        out_specs=(P("tp", "fs", None), P(None, "fs"), P("fs", None)),
        check_vma=False,
    )
```
